32 devices in a mesh: sp: 4 (over z), fs: 4 (over y, x), tp: 2 (over core).
Axes of the slice: x: 2, y: 2, z: 4, core: 2. Of those that a mesh axis runs over, the one named last changes fastest.
Arguments:
- tokens: bfloat16 [4, 1024, 2048], P('fs', ('sp', 'tp')), may hold values from -6 to 6
- query_weight: bfloat16 [2048, 2048], P(('sp', 'fs'), 'tp'), may hold values from -0.125 to 0.125
- forget_weight: bfloat16 [2048, 2048], P(('sp', 'fs'), 'tp'), may hold values from -0.125 to 0.125
- value_weight: bfloat16 [2048, 2048], P(('sp', 'fs'), 'tp'), may hold values from -0.125 to 0.125
- convolution_gate_weight: bfloat16 [2048, 1024], P(('sp', 'fs'), 'tp'), may hold values from -0.125 to 0.125
- convolution_multiplier_weight: bfloat16 [2048, 1024], P(('sp', 'fs'), 'tp'), may hold values from -0.125 to 0.125
- convolution_input_weight: bfloat16 [2048, 1024], P(('sp', 'fs'), 'tp'), may hold values from -0.125 to 0.125
- gate_headroom: float32 [2048], P('tp'), may hold values from 9.765625e-05 to 0.06
- added_log_rate: float32 [4, 16, 1024], P('fs', 'tp', 'sp'), may hold values from -1.6 to 0
- initial_state: float32 [4, 16, 128, 128], P('fs', 'tp'), may hold values from -0.5 to 0.5
- head_norm_gain: float32 [2048], P('tp'), may hold values from 0.1 to 1.9
- convolution_taps: float32 [3, 1024], P(None, 'tp'), may hold values from -3.5 to 3.5
- convolution_bias: float32 [1024], P('tp'), may hold values from -4 to 4
- recurrence_output_weight: bfloat16 [2048, 2048], P('tp', ('sp', 'fs')), may hold values from -0.109375 to 0.109375
- convolution_output_weight: bfloat16 [1024, 2048], P('tp', ('sp', 'fs')), may hold values from -0.109375 to 0.109375
Outputs:
- mixed: bfloat16 [4, 1024, 2048], P('fs', ('sp', 'tp'))
The draws below stay inside these ranges and needn't reach their ends.
All inputs are finite; a program needn't handle non-finite values.
Results may differ from the reference program's by a relative error of at most 0.018.
Values may be sent and summed in bfloat16 or wider, within the bound.
No kernel may reach another device: no remote copies, remote signals or barrier semaphores. Data moves between devices by JAX's collectives and lax.ppermute only.
A program may use at most 64 MiB of HBM per device.

```python
import jax
import jax.numpy as jnp
from jax import lax

D = 2048
RECURRENCE_HEADS = 16
DK = 128
CV = 1024
KW = 3
BLOCK_POSITIONS = 64
TOK = 256
HK = 2048
SEQ = 1024
BATCH = 4
N_TP = 2


def draw_gate_headroom(key, part):
    key_order, key_slow, key_fast = jax.random.split(jax.random.fold_in(key, 11), 3)
    head_order = jax.random.permutation(key_order, RECURRENCE_HEADS)
    slow_count = RECURRENCE_HEADS // 2
    slow_low = 0.25
    slow_high = 1.0
    slow_head = head_order < slow_count
    unit_slow = jax.random.uniform(key_slow, (RECURRENCE_HEADS, DK), jnp.float32)
    unit_fast = jax.random.uniform(key_fast, (RECURRENCE_HEADS, DK), jnp.float32)
    slow_gap = jnp.exp(jnp.log(slow_low) + unit_slow * (jnp.log(slow_high) - jnp.log(slow_low))) / SEQ
    fast_gap = jnp.exp(jnp.log(0.02) + unit_fast * (jnp.log(0.06) - jnp.log(0.02)))
    return jnp.where(slow_head[:, None], slow_gap, fast_gap).reshape(RECURRENCE_HEADS * DK).astype(jnp.float32)


def draw_added_log_rate(key, part):
    key_rate, key_spot, key_kept = jax.random.split(jax.random.fold_in(key, 23), 3)
    span_count = SEQ // TOK
    rate_low = 0.25
    rate_high = 1.0
    block_unit = jax.random.uniform(key_rate, (BATCH, 1, span_count, 1), jnp.float32)
    block_rate = jnp.exp(jnp.log(rate_low) + block_unit * (jnp.log(rate_high) - jnp.log(rate_low))) / SEQ
    stable_part = jnp.broadcast_to(-block_rate, (BATCH, RECURRENCE_HEADS, span_count, TOK)).reshape(BATCH, RECURRENCE_HEADS, SEQ)
    spots = jax.random.randint(key_spot, (BATCH, RECURRENCE_HEADS, 2), 0, SEQ)
    retained_fraction = jax.random.uniform(key_kept, (BATCH, RECURRENCE_HEADS, 2), jnp.float32, minval=0.5, maxval=0.8)
    at_location = jnp.arange(SEQ)[None, None, :, None] == spots[:, :, None, :]
    extra_log_rate = jnp.sum(jnp.where(at_location, jnp.log(retained_fraction)[:, :, None, :], 0.0), axis=-1)
    return (stable_part + extra_log_rate).astype(jnp.float32)


def block_scale(own_key, extent, cuts, low, largest):
    loudness, own = 1.0, jax.random.fold_in(own_key, 6)
    for dim, shards_of in cuts:
        draws = jnp.exp(jax.random.uniform(jax.random.fold_in(own, dim), (shards_of,), jnp.float32, low / len(cuts), largest / len(cuts)))
        loudness = loudness * jnp.repeat(draws, extent[dim] // shards_of).reshape([-1 if axis == dim else 1 for axis in range(len(extent))])
    return loudness


def bell_draw(key, dims, scale, limit, cuts=(), kind=jnp.bfloat16):
    gain = block_scale(key, dims, cuts, -0.22, 0.18) if cuts else 1.0
    entries = jax.random.normal(key, dims, jnp.float32) * scale * gain
    return jnp.minimum(jnp.maximum(entries, -limit), limit).astype(kind)


def setup_inputs(seed: int = 0) -> dict:
    streams_of = jax.random.split(jax.random.key(seed), 16)
    tokens = bell_draw(streams_of[0], (BATCH, SEQ, D), 1.0, 6.0, ((0, 4), (1, 8)))
    query_weight = bell_draw(streams_of[1], (D, HK), D ** -0.5, 0.125, ((0, 16), (1, 2)))
    forget_weight = bell_draw(streams_of[2], (D, HK), D ** -0.5, 0.125, ((0, 16), (1, 2)))
    value_weight = bell_draw(streams_of[3], (D, HK), D ** -0.5, 0.125, ((0, 16), (1, 2)))
    convolution_gate_weight = bell_draw(streams_of[4], (D, CV), D ** -0.5, 0.125, ((0, 16), (1, 2)))
    convolution_multiplier_weight = bell_draw(streams_of[5], (D, CV), D ** -0.5, 0.125, ((0, 16), (1, 2)))
    convolution_input_weight = bell_draw(streams_of[6], (D, CV), D ** -0.5, 0.125, ((0, 16), (1, 2)))
    gate_headroom = draw_gate_headroom(jax.random.fold_in(streams_of[15], 71), 0)
    added_log_rate = draw_added_log_rate(jax.random.fold_in(streams_of[15], 71), 0)
    initial_state = bell_draw(streams_of[9], (BATCH, RECURRENCE_HEADS, DK, DK), (SEQ ** -0.5), 0.5, ((0, 4), (1, 2)), jnp.float32)
    head_norm_gain = jnp.clip(1.0 + 0.18 * jax.random.normal(streams_of[10], (HK,), jnp.float32), 0.1, 1.9)
    convolution_taps = bell_draw(streams_of[11], (KW, CV), KW ** -0.5, 3.5, ((1, 2),), jnp.float32)
    convolution_bias = bell_draw(streams_of[12], (CV,), 1.0, 4.0, ((0, 2),), jnp.float32)
    recurrence_output_weight = bell_draw(streams_of[13], (HK, D), (HK + CV) ** -0.5, 0.109375, ((0, 2), (1, 16)))
    convolution_output_weight = bell_draw(streams_of[14], (CV, D), (HK + CV) ** -0.5, 0.109375, ((0, 2), (1, 16)))
    return {"tokens": tokens, "query_weight": query_weight, "forget_weight": forget_weight, "value_weight": value_weight, "convolution_gate_weight": convolution_gate_weight, "convolution_multiplier_weight": convolution_multiplier_weight, "convolution_input_weight": convolution_input_weight, "gate_headroom": gate_headroom, "added_log_rate": added_log_rate, "initial_state": initial_state, "head_norm_gain": head_norm_gain, "convolution_taps": convolution_taps, "convolution_bias": convolution_bias, "recurrence_output_weight": recurrence_output_weight, "convolution_output_weight": convolution_output_weight}


def project(sequence_rows, weight):
    return jnp.dot(sequence_rows, weight, preferred_element_type=jnp.float32).astype(jnp.bfloat16)

def to_blocks(values, number_of_blocks):
    return jnp.transpose(values.reshape(number_of_blocks, BLOCK_POSITIONS, RECURRENCE_HEADS, DK), (2, 0, 1, 3))

def gated_recurrence(query_vectors, forget_logits, value_vectors, gate_headroom, extra_rates, opening_state):
    length = query_vectors.shape[0]
    number_of_blocks = length // BLOCK_POSITIONS
    query_scaled = to_blocks(query_vectors.astype(jnp.float32), number_of_blocks) * DK ** (-0.5)
    gated_key = to_blocks(gate_headroom[None, :] * jax.nn.sigmoid(-forget_logits.astype(jnp.float32)), number_of_blocks)
    forget_log_rate = jnp.log1p(-gated_key) + extra_rates.reshape(RECURRENCE_HEADS, number_of_blocks, BLOCK_POSITIONS)[..., None]
    values = to_blocks(value_vectors.astype(jnp.float32), number_of_blocks)
    cumulative = jnp.cumsum(forget_log_rate, axis=2)
    query_decayed = query_scaled * jnp.exp(cumulative)
    key_decayed = gated_key * jnp.exp(-cumulative)
    scores = jnp.einsum('hnik,hnjk->hnij', query_decayed, key_decayed, precision=lax.Precision.HIGHEST)
    causal = jnp.tril(jnp.ones((BLOCK_POSITIONS, BLOCK_POSITIONS), dtype=bool))
    scores = jnp.where(causal, scores, 0.0)
    within = jnp.einsum('hnij,hnjv->hniv', scores, values, precision=lax.Precision.HIGHEST)
    final_log = cumulative[:, :, -1:, :]
    contrib = jnp.einsum('hnck,hncv->hnkv', gated_key * jnp.exp(final_log - cumulative), values, precision=lax.Precision.HIGHEST)
    decays = jnp.exp(final_log[:, :, 0, :])

    def advance(current, block_pair):
        return (block_pair[0][..., None] * current + block_pair[1], current)
    _, entering = lax.scan(advance, opening_state, (jnp.moveaxis(decays, 1, 0), jnp.moveaxis(contrib, 1, 0)))
    entering = jnp.moveaxis(entering, 0, 1)
    carried_term = jnp.einsum('hnck,hnkv->hncv', query_decayed, entering, precision=lax.Precision.HIGHEST)
    return jnp.transpose(within + carried_term, (1, 2, 0, 3)).reshape(length, RECURRENCE_HEADS, DK)

def reference(tokens, query_weight, forget_weight, value_weight, convolution_gate_weight, convolution_multiplier_weight, convolution_input_weight, gate_headroom, added_log_rate, initial_state, head_norm_gain, convolution_taps, convolution_bias, recurrence_output_weight, convolution_output_weight):

    def single_sequence(input_rows):
        sequence_rows, extra_rates, opening_state = input_rows
        length = sequence_rows.shape[0]
        query_vectors = project(sequence_rows, query_weight)
        forget_logits = project(sequence_rows, forget_weight)
        value_vectors = project(sequence_rows, value_weight)
        conv_gate = project(sequence_rows, convolution_gate_weight)
        conv_mult = project(sequence_rows, convolution_multiplier_weight)
        conv_input = project(sequence_rows, convolution_input_weight)
        recurrence_unnormed = gated_recurrence(query_vectors, forget_logits, value_vectors, gate_headroom, extra_rates, opening_state)
        mean_square = lax.optimization_barrier(jnp.mean(recurrence_unnormed * recurrence_unnormed, axis=-1, keepdims=True))
        rec_out = recurrence_unnormed * lax.rsqrt(mean_square + 1e-06) * head_norm_gain.reshape(RECURRENCE_HEADS, DK)
        rec_out = rec_out.reshape(length, HK).astype(jnp.bfloat16)
        conv_prod = conv_mult.astype(jnp.float32) * conv_input.astype(jnp.float32)
        padded = jnp.concatenate([jnp.zeros((KW - 1, CV), jnp.float32), conv_prod], axis=0)
        conv_y = jnp.broadcast_to(convolution_bias[None, :], (length, CV))
        for j in range(KW):
            conv_y = conv_y + convolution_taps[j][None, :] * padded[j:j + length]
        conv_out = (conv_gate.astype(jnp.float32) * conv_y).astype(jnp.bfloat16)
        rec_group = HK // N_TP
        conv_group = CV // N_TP
        running = jnp.zeros((length, D), jnp.float32)
        for g in range(N_TP):
            partial_value = jnp.dot(rec_out[:, g * rec_group:(g + 1) * rec_group], recurrence_output_weight[g * rec_group:(g + 1) * rec_group], preferred_element_type=jnp.float32)
            partial_value = partial_value + jnp.dot(conv_out[:, g * conv_group:(g + 1) * conv_group], convolution_output_weight[g * conv_group:(g + 1) * conv_group], preferred_element_type=jnp.float32)
            running = running + lax.optimization_barrier(partial_value.astype(jnp.bfloat16)).astype(jnp.float32)
        return running.astype(jnp.bfloat16)
    return lax.map(single_sequence, (tokens, added_log_rate, initial_state))
```

```python
import jax
import jax.numpy as jnp
from jax import lax
from jax.experimental import pallas as pl
from jax.experimental.pallas import tpu as pltpu
from jax.sharding import PartitionSpec as P

DK = 128
KW = 3
BLOCK_POSITIONS = 64


def carried_in(part, axis, combine, identity):
    place = lax.axis_index(axis)
    gathered = jax.tree.map(lambda a: lax.all_gather(a, axis), part)
    state = jax.tree.map(lambda a, e: jnp.zeros_like(a) + jnp.asarray(e, a.dtype), part, identity)

    def one(hop, state):
        return combine(
            state, jax.tree.map(lambda a: lax.dynamic_index_in_dim(a, hop, 0, False), gathered)
        )

    return lax.fori_loop(0, place, one, state)


def from_behind(block, axis, distance):
    devices = range(lax.axis_size(axis))
    route = [(i - distance, i) for i in devices if i - distance in devices]
    return lax.ppermute(block, axis, route)


def to_blocks(values, number_of_heads):
    number_of_blocks = values.shape[0] // BLOCK_POSITIONS
    return jnp.transpose(
        values.reshape(number_of_blocks, BLOCK_POSITIONS, number_of_heads, DK), (2, 0, 1, 3)
    )


def within_block_recurrence(
    query_vectors, forget_logits, value_vectors, gate_headroom, extra_rates
):
    number_of_heads = extra_rates.shape[0]
    number_of_blocks = query_vectors.shape[0] // BLOCK_POSITIONS
    query_scaled = to_blocks(query_vectors.astype(jnp.float32), number_of_heads) * DK ** (-0.5)
    gated_key = to_blocks(
        gate_headroom[None, :] * jax.nn.sigmoid(-forget_logits.astype(jnp.float32)), number_of_heads
    )
    forget_log_rate = (
        jnp.log1p(-gated_key)
        + extra_rates.reshape(number_of_heads, number_of_blocks, BLOCK_POSITIONS)[..., None]
    )
    values = to_blocks(value_vectors.astype(jnp.float32), number_of_heads)
    cumulative = jnp.cumsum(forget_log_rate, axis=2)
    query_decayed = query_scaled * jnp.exp(cumulative)
    key_decayed = gated_key * jnp.exp(-cumulative)
    scores = jnp.einsum(
        "hnik,hnjk->hnij", query_decayed, key_decayed, precision=lax.Precision.HIGHEST
    )
    causal = jnp.tril(jnp.ones((BLOCK_POSITIONS, BLOCK_POSITIONS), dtype=bool))
    scores = jnp.where(causal, scores, 0.0)
    within = jnp.einsum("hnij,hnjv->hniv", scores, values, precision=lax.Precision.HIGHEST)
    final_log = cumulative[:, :, -1, :]
    contrib = jnp.einsum(
        "hnck,hncv->hnkv",
        gated_key * jnp.exp(final_log[:, :, None, :] - cumulative),
        values,
        precision=lax.Precision.HIGHEST,
    )
    decays = jnp.exp(final_log)

    def advance(current, block_pair):
        return (block_pair[0][..., None] * current + block_pair[1], current)

    empty_state = jnp.zeros((number_of_heads, DK, DK), jnp.float32)
    local_total, entering = lax.scan(
        advance, empty_state, (jnp.moveaxis(decays, 1, 0), jnp.moveaxis(contrib, 1, 0))
    )
    entering = jnp.moveaxis(entering, 0, 1)
    before = jnp.exp(jnp.cumsum(final_log, axis=1) - final_log)
    device_decay = jnp.exp(jnp.sum(final_log, axis=1))
    return (query_decayed, within, entering, before, device_decay, local_total)


def finish(query_decayed, within, entering, before, carried, head_norm_gain):
    number_of_heads = query_decayed.shape[0]
    states = entering + before[..., None] * carried[:, None]
    carried_term = jnp.einsum(
        "hnck,hnkv->hncv", query_decayed, states, precision=lax.Precision.HIGHEST
    )
    length = query_decayed.shape[1] * BLOCK_POSITIONS
    recurrence_unnormed = jnp.transpose(within + carried_term, (1, 2, 0, 3)).reshape(
        length, number_of_heads, DK
    )
    mean_square = jnp.mean(recurrence_unnormed * recurrence_unnormed, axis=-1, keepdims=True)
    rec_out = (
        recurrence_unnormed
        * lax.rsqrt(mean_square + 1e-06)
        * head_norm_gain.reshape(number_of_heads, DK)
    )
    return rec_out.reshape(length, number_of_heads * DK).astype(jnp.bfloat16)


def chain_combine(earlier_part, later_part):
    return (
        earlier_part[0] * later_part[0],
        later_part[0][..., None] * earlier_part[1] + later_part[1],
    )


def shards(
    tokens,
    query_weight,
    forget_weight,
    value_weight,
    convolution_gate_weight,
    convolution_multiplier_weight,
    convolution_input_weight,
    gate_headroom,
    added_log_rate,
    initial_state,
    head_norm_gain,
    convolution_taps,
    convolution_bias,
    recurrence_output_weight,
    convolution_output_weight,
):
    own_rows = tokens[0]
    gathered = (
        lax.all_gather(query_weight, ("sp", "fs"), axis=0, tiled=True),
        lax.all_gather(forget_weight, ("sp", "fs"), axis=0, tiled=True),
        lax.all_gather(value_weight, ("sp", "fs"), axis=0, tiled=True),
        lax.all_gather(convolution_gate_weight, ("sp", "fs"), axis=0, tiled=True),
        lax.all_gather(convolution_multiplier_weight, ("sp", "fs"), axis=0, tiled=True),
        lax.all_gather(convolution_input_weight, ("sp", "fs"), axis=0, tiled=True),
        lax.all_gather(recurrence_output_weight, ("sp", "fs"), axis=1, tiled=True),
        lax.all_gather(convolution_output_weight, ("sp", "fs"), axis=1, tiled=True),
    )
    in_weights = gathered[:6]
    out_rec = gathered[6]
    out_conv = gathered[7]
    block_rows = lax.all_gather(own_rows, "tp", axis=0, tiled=True)
    projected = jnp.concatenate(
        [
            jnp.dot(block_rows, weight, preferred_element_type=jnp.float32).astype(jnp.bfloat16)
            for weight in in_weights
        ],
        axis=1,
    )
    rec_width = query_weight.shape[1]
    conv_width = convolution_gate_weight.shape[1]
    query_vectors = projected[:, :rec_width]
    forget_logits = projected[:, rec_width : 2 * rec_width]
    value_vectors = projected[:, 2 * rec_width : 3 * rec_width]
    conv_base = 3 * rec_width
    conv_gate = projected[:, conv_base : conv_base + conv_width]
    conv_mult = projected[:, conv_base + conv_width : conv_base + 2 * conv_width]
    conv_input = projected[:, conv_base + 2 * conv_width : conv_base + 3 * conv_width]
    query_decayed, within, entering, before, device_decay, local_total = within_block_recurrence(
        query_vectors, forget_logits, value_vectors, gate_headroom, added_log_rate[0]
    )
    conv_prod = conv_mult.astype(jnp.float32) * conv_input.astype(jnp.float32)
    length = conv_prod.shape[0]
    tail_rows = conv_prod[length - (KW - 1) :]
    unit_decay = jnp.ones_like(device_decay)
    empty_state = jnp.zeros_like(local_total)
    prior_decay, prior_state = carried_in(
        (device_decay, local_total), "sp", chain_combine, (unit_decay, empty_state)
    )
    prior_rows = from_behind(tail_rows, "sp", 1)
    carried = prior_decay[..., None] * initial_state[0] + prior_state
    rec_out = finish(query_decayed, within, entering, before, carried, head_norm_gain)
    extended = jnp.concatenate([prior_rows, conv_prod], axis=0)
    conv_y = jnp.broadcast_to(convolution_bias[None, :], conv_prod.shape)
    for j in range(KW):
        conv_y = conv_y + convolution_taps[j][None, :] * extended[j : j + length]
    conv_out = (conv_gate.astype(jnp.float32) * conv_y).astype(jnp.bfloat16)
    mixed = lax.psum_scatter(
        (
            jnp.dot(rec_out, out_rec, preferred_element_type=jnp.float32)
            + jnp.dot(conv_out, out_conv, preferred_element_type=jnp.float32)
        ).astype(jnp.bfloat16),
        "tp",
        scatter_dimension=0,
        tiled=True,
    )
    return mixed[None]


def flip(value, axis, mask):
    return lax.ppermute(value, axis, [(i, i ^ mask) for i in range(lax.axis_size(axis))])


def shift(value, axis, distance):
    n = lax.axis_size(axis)
    return lax.ppermute(value, axis, [(i, (i + distance) % n) for i in range(n)])


def ring_exchange(pieces, axis):
    place = lax.axis_index(axis)

    def for_offset(offset):
        return lax.dynamic_index_in_dim(pieces, (place + offset) % 4, 0, False)

    across = for_offset(2)
    half = across.shape[0] // 2
    up = shift(jnp.concatenate([for_offset(1), across[:half]], axis=0), axis, 1)
    down = shift(jnp.concatenate([for_offset(3), across[half:]], axis=0), axis, -1)
    rows = pieces.shape[1]
    far_up = shift(up[rows:], axis, 1)
    far_down = shift(down[rows:], axis, -1)
    return [for_offset(0), down[:rows], jnp.concatenate([far_up, far_down], axis=0), up[:rows]]


def in_order(by_offset, axis):
    place = lax.axis_index(axis)
    n = len(by_offset)
    stacked = jnp.stack(list(by_offset) + list(by_offset)[: n - 1])
    return lax.dynamic_slice_in_dim(stacked, (n - place) % n, n, 0)


def ring_gather(block, axis):
    half = block.shape[0] // 2
    below = shift(block, axis, 1)
    above = shift(block, axis, -1)
    far = jnp.concatenate([shift(below[:half], axis, 1), shift(above[half:], axis, -1)], axis=0)
    return [block, above, far, below]


def square_gather(block, axis):
    half = block.shape[0] // 2
    one = flip(block, axis, 1)
    two = flip(block, axis, 2)
    three = jnp.concatenate([flip(two[:half], axis, 1), flip(one[half:], axis, 2)], axis=0)
    return [block, one, two, three]


def recurrence_kernel(q_ref, f_ref, v_ref, headroom_ref, rate_ref, state_ref, gain_ref, out_ref):
    length, width = q_ref.shape
    heads = width // DK
    step = BLOCK_POSITIONS
    row = lax.broadcasted_iota(jnp.int32, (step, step), 0)
    col = lax.broadcasted_iota(jnp.int32, (step, step), 1)
    causal = row >= col
    ones = jnp.where(causal, 1.0, 0.0).astype(jnp.float32)
    contract_last = (((1,), (1,)), ((), ()))
    contract_first = (((0,), (0,)), ((), ()))
    dot = lambda a, b, dims: lax.dot_general(a, b, dims, preferred_element_type=jnp.float32)

    def advance(n, states):
        start = pl.multiple_of(n * step, step)
        span = pl.ds(start, step)
        following = []
        for h in range(heads):
            lanes = pl.ds(h * DK, DK)
            state = states[h]
            logits = f_ref[span, lanes].astype(jnp.float32)
            key = headroom_ref[:, lanes] * jax.nn.sigmoid(-logits)
            rate = jnp.log1p(-key) + rate_ref[span, h : h + 1]
            cumulative = lax.dot_general(
                ones,
                rate,
                (((1,), (0,)), ((), ())),
                precision=lax.Precision.HIGHEST,
                preferred_element_type=jnp.float32,
            )
            middle = cumulative[step // 2 - 1 : step // 2]
            final = cumulative[step - 1 : step]
            query = q_ref[span, lanes].astype(jnp.float32) * DK ** (-0.5)
            value = v_ref[span, lanes]
            scores = dot(
                (query * jnp.exp(cumulative - middle)).astype(jnp.bfloat16),
                (key * jnp.exp(middle - cumulative)).astype(jnp.bfloat16),
                contract_last,
            )
            scores = jnp.where(causal, scores, 0.0).astype(jnp.bfloat16)
            raw = dot(scores, value, (((1,), (0,)), ((), ()))) + dot(
                (query * jnp.exp(cumulative)).astype(jnp.bfloat16),
                state.astype(jnp.bfloat16),
                contract_last,
            )
            contrib = dot(
                value, (key * jnp.exp(final - cumulative)).astype(jnp.bfloat16), contract_first
            )
            following.append(jnp.exp(final) * state + contrib)
            mean_square = jnp.mean(raw * raw, axis=-1, keepdims=True)
            out_ref[span, lanes] = (
                raw * lax.rsqrt(mean_square + 1e-06) * gain_ref[:, lanes]
            ).astype(jnp.bfloat16)
        return tuple(following)

    lax.fori_loop(
        0, length // step, advance, tuple(state_ref[h] for h in range(heads)), unroll=2
    )


def recurrence(query, forget, value, headroom, rates, state, gain):
    return pl.pallas_call(
        recurrence_kernel,
        out_shape=jax.ShapeDtypeStruct(query.shape, jnp.bfloat16),
        name="recurrence",
    )(
        query,
        forget,
        value,
        headroom[None, :],
        rates.T,
        jnp.swapaxes(state, 1, 2),
        gain[None, :],
    )


def by_heads_shards(
    tokens,
    query_weight,
    forget_weight,
    value_weight,
    convolution_gate_weight,
    convolution_multiplier_weight,
    convolution_input_weight,
    gate_headroom,
    added_log_rate,
    initial_state,
    head_norm_gain,
    convolution_taps,
    convolution_bias,
    recurrence_output_weight,
    convolution_output_weight,
):
    n_sp = lax.axis_size("sp")
    n_fs = lax.axis_size("fs")
    place = lax.axis_index("sp")
    square = lax.axis_index("fs")
    core = lax.axis_index("tp")
    own_rows = tokens[0]
    row_count = query_weight.shape[0]
    out_cols = recurrence_output_weight.shape[1]

    def own(value, axis):
        size = value.shape[axis] // n_sp
        return lax.dynamic_slice_in_dim(value, place * size, size, axis)

    def columns(weights):
        parts = [w.reshape(row_count, n_sp, w.shape[1] // n_sp) for w in weights]
        return jnp.swapaxes(jnp.concatenate(parts, axis=2), 0, 1)

    first = columns((query_weight, forget_weight, value_weight))
    second = columns(
        (convolution_gate_weight, convolution_multiplier_weight, convolution_input_weight)
    )
    third = jnp.concatenate(
        [
            w.reshape(n_sp, w.shape[0] // n_sp, out_cols)
            for w in (recurrence_output_weight, convolution_output_weight)
        ],
        axis=1,
    )
    blocks = own_rows.reshape(own_rows.shape[0], n_sp, n_fs, row_count)
    sorted_rows = jnp.concatenate(
        [lax.dynamic_index_in_dim(blocks, square ^ j, 2, False)[:, None] for j in range(n_fs)],
        axis=1,
    ).reshape(own_rows.shape)

    def gathered(pieces):
        mine = in_order(ring_exchange(pieces, "sp"), "sp")
        return square_gather(mine, "fs")

    first_parts = gathered(first)
    row_blocks = in_order(ring_gather(sorted_rows, "sp"), "sp")
    other_blocks = flip(row_blocks, "tp", 1)
    even = jnp.where(core == 0, row_blocks, other_blocks)
    odd = jnp.where(core == 0, other_blocks, row_blocks)
    all_rows = jnp.stack([even, odd], axis=1).reshape(-1, own_rows.shape[1])
    second_parts = gathered(second)
    third_parts = gathered(third)

    def project(parts):
        weight = jnp.concatenate([p.reshape(-1, p.shape[-1]) for p in parts], axis=0)
        return jnp.dot(all_rows, weight, preferred_element_type=jnp.float32).astype(jnp.bfloat16)

    head_cols = query_weight.shape[1] // n_sp
    recurrent = project(first_parts)
    rec_out = recurrence(
        recurrent[:, :head_cols],
        recurrent[:, head_cols : 2 * head_cols],
        recurrent[:, 2 * head_cols :],
        own(gate_headroom, 0),
        own(rates_of(added_log_rate), 0),
        own(initial_state[0], 0),
        own(head_norm_gain, 0),
    )
    conv_cols = convolution_gate_weight.shape[1] // n_sp
    short = project(second_parts)
    conv_gate = short[:, :conv_cols].astype(jnp.float32)
    conv_prod = short[:, conv_cols : 2 * conv_cols].astype(jnp.float32) * short[
        :, 2 * conv_cols :
    ].astype(jnp.float32)
    length = conv_prod.shape[0]
    extended = jnp.concatenate([jnp.zeros((KW - 1, conv_cols), jnp.float32), conv_prod], axis=0)
    taps = own(convolution_taps, 1)
    conv_y = jnp.broadcast_to(own(convolution_bias, 0)[None, :], conv_prod.shape)
    for j in range(KW):
        conv_y = conv_y + taps[j][None, :] * extended[j : j + length]
    conv_out = (conv_gate * conv_y).astype(jnp.bfloat16)
    mixed_in = jnp.concatenate([rec_out, conv_out], axis=1)
    out_weight = jnp.concatenate(
        [p[s] for p in third_parts for s in range(n_sp)], axis=1
    )
    partial = jnp.dot(mixed_in, out_weight, preferred_element_type=jnp.float32).astype(
        jnp.bfloat16
    )
    spans = partial.reshape(n_sp, 2, own_rows.shape[0], partial.shape[1])
    kept = lax.dynamic_index_in_dim(spans, core, 1, False)
    sent = lax.dynamic_index_in_dim(spans, 1 - core, 1, False)
    pair = (kept.astype(jnp.float32) + flip(sent, "tp", 1).astype(jnp.float32)).astype(jnp.bfloat16)
    total = sum(part.astype(jnp.float32) for part in ring_exchange(pair, "sp"))
    total = total.astype(jnp.bfloat16).reshape(-1, n_fs, n_sp, out_cols)
    mixed = jnp.stack(
        [lax.dynamic_index_in_dim(total, square ^ j, 1, False) for j in range(n_fs)], axis=2
    )
    return mixed.reshape(own_rows.shape)[None]


def rates_of(added_log_rate):
    return lax.all_gather(added_log_rate[0], "sp", axis=1, tiled=True)


def solution(mesh):
    in_specs = (
        P("fs", ("sp", "tp"), None),
        P(("sp", "fs"), "tp"),
        P(("sp", "fs"), "tp"),
        P(("sp", "fs"), "tp"),
        P(("sp", "fs"), "tp"),
        P(("sp", "fs"), "tp"),
        P(("sp", "fs"), "tp"),
        P("tp"),
        P("fs", "tp", "sp"),
        P("fs", "tp", None, None),
        P("tp"),
        P(None, "tp"),
        P("tp"),
        P("tp", ("sp", "fs")),
        P("tp", ("sp", "fs")),
    )
    out_specs = P("fs", ("sp", "tp"), None)
    sizes = dict(mesh.shape)

    def run(*arrays):
        heads = arrays[8].shape[1] // sizes["tp"]
        channels = arrays[4].shape[1] // sizes["tp"]
        by_heads = (
            (sizes["sp"], sizes["fs"], sizes["tp"]) == (4, 4, 2)
            and heads % sizes["sp"] == 0
            and channels % (128 * sizes["sp"]) == 0
        )
        return jax.shard_map(
            by_heads_shards if by_heads else shards,
            mesh=mesh,
            in_specs=in_specs,
            out_specs=out_specs,
            check_vma=False,
        )(*arrays)

    return run
```

```python
import functools

import jax
import jax.numpy as jnp
from jax import lax
from jax.experimental import pallas as pl
from jax.experimental.pallas import tpu as pltpu
from jax.sharding import PartitionSpec as P

DK = 128
KW = 3
BLOCK_POSITIONS = 64


def carried_in(part, axis, combine, identity):
    place = lax.axis_index(axis)
    gathered = jax.tree.map(lambda a: lax.all_gather(a, axis), part)
    state = jax.tree.map(lambda a, e: jnp.zeros_like(a) + jnp.asarray(e, a.dtype), part, identity)

    def one(hop, state):
        return combine(
            state, jax.tree.map(lambda a: lax.dynamic_index_in_dim(a, hop, 0, False), gathered)
        )

    return lax.fori_loop(0, place, one, state)


def from_behind(block, axis, distance):
    devices = range(lax.axis_size(axis))
    route = [(i - distance, i) for i in devices if i - distance in devices]
    return lax.ppermute(block, axis, route)


def to_blocks(values, number_of_heads):
    number_of_blocks = values.shape[0] // BLOCK_POSITIONS
    return jnp.transpose(
        values.reshape(number_of_blocks, BLOCK_POSITIONS, number_of_heads, DK), (2, 0, 1, 3)
    )


def within_block_recurrence(
    query_vectors, forget_logits, value_vectors, gate_headroom, extra_rates
):
    number_of_heads = extra_rates.shape[0]
    number_of_blocks = query_vectors.shape[0] // BLOCK_POSITIONS
    query_scaled = to_blocks(query_vectors.astype(jnp.float32), number_of_heads) * DK ** (-0.5)
    gated_key = to_blocks(
        gate_headroom[None, :] * jax.nn.sigmoid(-forget_logits.astype(jnp.float32)), number_of_heads
    )
    forget_log_rate = (
        jnp.log1p(-gated_key)
        + extra_rates.reshape(number_of_heads, number_of_blocks, BLOCK_POSITIONS)[..., None]
    )
    values = to_blocks(value_vectors.astype(jnp.float32), number_of_heads)
    cumulative = jnp.cumsum(forget_log_rate, axis=2)
    query_decayed = query_scaled * jnp.exp(cumulative)
    key_decayed = gated_key * jnp.exp(-cumulative)
    scores = jnp.einsum(
        "hnik,hnjk->hnij", query_decayed, key_decayed, precision=lax.Precision.HIGHEST
    )
    causal = jnp.tril(jnp.ones((BLOCK_POSITIONS, BLOCK_POSITIONS), dtype=bool))
    scores = jnp.where(causal, scores, 0.0)
    within = jnp.einsum("hnij,hnjv->hniv", scores, values, precision=lax.Precision.HIGHEST)
    final_log = cumulative[:, :, -1, :]
    contrib = jnp.einsum(
        "hnck,hncv->hnkv",
        gated_key * jnp.exp(final_log[:, :, None, :] - cumulative),
        values,
        precision=lax.Precision.HIGHEST,
    )
    decays = jnp.exp(final_log)

    def advance(current, block_pair):
        return (block_pair[0][..., None] * current + block_pair[1], current)

    empty_state = jnp.zeros((number_of_heads, DK, DK), jnp.float32)
    local_total, entering = lax.scan(
        advance, empty_state, (jnp.moveaxis(decays, 1, 0), jnp.moveaxis(contrib, 1, 0))
    )
    entering = jnp.moveaxis(entering, 0, 1)
    before = jnp.exp(jnp.cumsum(final_log, axis=1) - final_log)
    device_decay = jnp.exp(jnp.sum(final_log, axis=1))
    return (query_decayed, within, entering, before, device_decay, local_total)


def finish(query_decayed, within, entering, before, carried, head_norm_gain):
    number_of_heads = query_decayed.shape[0]
    states = entering + before[..., None] * carried[:, None]
    carried_term = jnp.einsum(
        "hnck,hnkv->hncv", query_decayed, states, precision=lax.Precision.HIGHEST
    )
    length = query_decayed.shape[1] * BLOCK_POSITIONS
    recurrence_unnormed = jnp.transpose(within + carried_term, (1, 2, 0, 3)).reshape(
        length, number_of_heads, DK
    )
    mean_square = jnp.mean(recurrence_unnormed * recurrence_unnormed, axis=-1, keepdims=True)
    rec_out = (
        recurrence_unnormed
        * lax.rsqrt(mean_square + 1e-06)
        * head_norm_gain.reshape(number_of_heads, DK)
    )
    return rec_out.reshape(length, number_of_heads * DK).astype(jnp.bfloat16)


def chain_combine(earlier_part, later_part):
    return (
        earlier_part[0] * later_part[0],
        later_part[0][..., None] * earlier_part[1] + later_part[1],
    )


def shards(
    tokens,
    query_weight,
    forget_weight,
    value_weight,
    convolution_gate_weight,
    convolution_multiplier_weight,
    convolution_input_weight,
    gate_headroom,
    added_log_rate,
    initial_state,
    head_norm_gain,
    convolution_taps,
    convolution_bias,
    recurrence_output_weight,
    convolution_output_weight,
):
    own_rows = tokens[0]
    gathered = (
        lax.all_gather(query_weight, ("sp", "fs"), axis=0, tiled=True),
        lax.all_gather(forget_weight, ("sp", "fs"), axis=0, tiled=True),
        lax.all_gather(value_weight, ("sp", "fs"), axis=0, tiled=True),
        lax.all_gather(convolution_gate_weight, ("sp", "fs"), axis=0, tiled=True),
        lax.all_gather(convolution_multiplier_weight, ("sp", "fs"), axis=0, tiled=True),
        lax.all_gather(convolution_input_weight, ("sp", "fs"), axis=0, tiled=True),
        lax.all_gather(recurrence_output_weight, ("sp", "fs"), axis=1, tiled=True),
        lax.all_gather(convolution_output_weight, ("sp", "fs"), axis=1, tiled=True),
    )
    in_weights = gathered[:6]
    out_rec = gathered[6]
    out_conv = gathered[7]
    block_rows = lax.all_gather(own_rows, "tp", axis=0, tiled=True)
    projected = jnp.concatenate(
        [
            jnp.dot(block_rows, weight, preferred_element_type=jnp.float32).astype(jnp.bfloat16)
            for weight in in_weights
        ],
        axis=1,
    )
    rec_width = query_weight.shape[1]
    conv_width = convolution_gate_weight.shape[1]
    query_vectors = projected[:, :rec_width]
    forget_logits = projected[:, rec_width : 2 * rec_width]
    value_vectors = projected[:, 2 * rec_width : 3 * rec_width]
    conv_base = 3 * rec_width
    conv_gate = projected[:, conv_base : conv_base + conv_width]
    conv_mult = projected[:, conv_base + conv_width : conv_base + 2 * conv_width]
    conv_input = projected[:, conv_base + 2 * conv_width : conv_base + 3 * conv_width]
    query_decayed, within, entering, before, device_decay, local_total = within_block_recurrence(
        query_vectors, forget_logits, value_vectors, gate_headroom, added_log_rate[0]
    )
    conv_prod = conv_mult.astype(jnp.float32) * conv_input.astype(jnp.float32)
    length = conv_prod.shape[0]
    tail_rows = conv_prod[length - (KW - 1) :]
    unit_decay = jnp.ones_like(device_decay)
    empty_state = jnp.zeros_like(local_total)
    prior_decay, prior_state = carried_in(
        (device_decay, local_total), "sp", chain_combine, (unit_decay, empty_state)
    )
    prior_rows = from_behind(tail_rows, "sp", 1)
    carried = prior_decay[..., None] * initial_state[0] + prior_state
    rec_out = finish(query_decayed, within, entering, before, carried, head_norm_gain)
    extended = jnp.concatenate([prior_rows, conv_prod], axis=0)
    conv_y = jnp.broadcast_to(convolution_bias[None, :], conv_prod.shape)
    for j in range(KW):
        conv_y = conv_y + convolution_taps[j][None, :] * extended[j : j + length]
    conv_out = (conv_gate.astype(jnp.float32) * conv_y).astype(jnp.bfloat16)
    mixed = lax.psum_scatter(
        (
            jnp.dot(rec_out, out_rec, preferred_element_type=jnp.float32)
            + jnp.dot(conv_out, out_conv, preferred_element_type=jnp.float32)
        ).astype(jnp.bfloat16),
        "tp",
        scatter_dimension=0,
        tiled=True,
    )
    return mixed[None]


def flip(value, axis, mask):
    return lax.ppermute(value, axis, [(i, i ^ mask) for i in range(lax.axis_size(axis))])


def shift(value, axis, distance):
    n = lax.axis_size(axis)
    return lax.ppermute(value, axis, [(i, (i + distance) % n) for i in range(n)])


def for_offsets(pieces, axis):
    place = lax.axis_index(axis)
    n = pieces.shape[0]
    return [lax.dynamic_index_in_dim(pieces, (place + k) % n, 0, False) for k in range(n)]


def exchange(by_offset, axis):
    n = len(by_offset)
    received = {k: shift(by_offset[k], axis, k) for k in range(1, n)}
    return [by_offset[0]] + [received[n - k] for k in range(1, n)]


def in_order(by_offset, axis):
    place = lax.axis_index(axis)
    n = len(by_offset)
    out = jnp.zeros((n,) + by_offset[0].shape, by_offset[0].dtype)
    for k in range(n):
        out = lax.dynamic_update_index_in_dim(out, by_offset[k], (place + k) % n, 0)
    return out


def square_gather(block, axis):
    half = block.shape[0] // 2
    one = flip(block, axis, 1)
    two = flip(block, axis, 2)
    three = jnp.concatenate([flip(two[:half], axis, 1), flip(one[half:], axis, 2)], axis=0)
    return [block, one, two, three]


def base_row(place_ref, m, length, rows):
    spans = length // (2 * rows)
    offset = (m // 2 + spans - place_ref[0]) % spans
    base = (m % 2 ^ place_ref[1]) * (length // 2) + offset * rows
    return base, offset * 2 * rows + m % 2 * rows


def project_into(scratch_ref, block_refs, weight_refs):
    for i, block_ref in enumerate(block_refs):
        rows, model = block_ref.shape
        group = model // len(weight_refs)
        total = 0.0
        for j, weight_ref in enumerate(weight_refs):
            weight = weight_ref[:, : group // weight_ref.shape[0], :]
            total = total + jnp.dot(
                block_ref[:, j * group : (j + 1) * group],
                weight.reshape(group, weight.shape[2]),
                preferred_element_type=jnp.float32,
            )
        scratch_ref[i * rows : (i + 1) * rows, :] = total.astype(jnp.bfloat16)


def recurrence_kernel(core_ref, *refs, rows, counts):
    n, k = counts
    headroom_ref, rate_ref, state_ref, gain_ref, out_ref, rec_ref = refs[n + k :]
    project_into(rec_ref, refs[:n], refs[n : n + k])
    length, width = out_ref.shape
    heads = width // DK
    step = BLOCK_POSITIONS
    base_of = lambda m: base_row(core_ref, m, length, rows)
    row = lax.broadcasted_iota(jnp.int32, (step, step), 0)
    col = lax.broadcasted_iota(jnp.int32, (step, step), 1)
    causal = row >= col
    ones = jnp.where(causal, 1.0, 0.0).astype(jnp.bfloat16)
    plain = (((1,), (0,)), ((), ()))
    contract_last = (((1,), (1,)), ((), ()))
    contract_first = (((0,), (0,)), ((), ()))
    dot = lambda a, b, dims: lax.dot_general(a, b, dims, preferred_element_type=jnp.float32)

    def one(state, h, span, position):
        lanes = slice(h * DK, (h + 1) * DK)
        logits = rec_ref[span, width + h * DK : width + (h + 1) * DK].astype(jnp.float32)
        key = headroom_ref[:, lanes] * jax.nn.sigmoid(-logits)
        rate = jnp.log1p(-key) + rate_ref[pl.ds(position, step), h : h + 1]
        high = rate.astype(jnp.bfloat16)
        rest = rate - high.astype(jnp.float32)
        middle = rest.astype(jnp.bfloat16)
        low = (rest - middle.astype(jnp.float32)).astype(jnp.bfloat16)
        cumulative = dot(ones, high, plain) + dot(ones, middle, plain) + dot(ones, low, plain)
        middle = cumulative[step // 2 - 1 : step // 2]
        final = cumulative[step - 1 : step]
        query = rec_ref[span, lanes].astype(jnp.float32) * DK ** (-0.5)
        value = rec_ref[span, 2 * width + h * DK : 2 * width + (h + 1) * DK]
        scores = dot(
            (query * jnp.exp(cumulative - middle)).astype(jnp.bfloat16),
            (key * jnp.exp(middle - cumulative)).astype(jnp.bfloat16),
            contract_last,
        )
        scores = jnp.where(causal, scores, 0.0).astype(jnp.bfloat16)
        raw = dot(scores, value, plain) + dot(
            (query * jnp.exp(cumulative)).astype(jnp.bfloat16),
            state.astype(jnp.bfloat16),
            contract_last,
        )
        contrib = dot(
            value, (key * jnp.exp(final - cumulative)).astype(jnp.bfloat16), contract_first
        )
        mean_square = jnp.mean(raw * raw, axis=-1, keepdims=True)
        out_ref[span, lanes] = (
            raw * lax.rsqrt(mean_square + 1e-06) * gain_ref[:, lanes]
        ).astype(jnp.bfloat16)
        return jnp.exp(final) * state + contrib

    def advance(m, states):
        base, rate_base = base_of(m)
        for b in range(rows // step):
            span = pl.ds(pl.multiple_of(base + b * step, step), step)
            position = pl.multiple_of(rate_base + b * step, step)
            states = tuple(one(states[h], h, span, position) for h in range(heads))
        return states

    lax.fori_loop(0, length // rows, advance, tuple(state_ref[h] for h in range(heads)))


def convolution_kernel(core_ref, *refs, rows, counts):
    n, k = counts
    taps_ref, bias_ref, out_ref, short_ref = refs[n + k :]
    project_into(short_ref, refs[:n], refs[n : n + k])
    length, width = out_ref.shape
    base_of = lambda m: base_row(core_ref, m, length, rows)
    row = lax.broadcasted_iota(jnp.int32, (rows, width), 0)

    def advance(m, before):
        base, _ = base_of(m)
        span = pl.ds(pl.multiple_of(base, rows), rows)
        gate = short_ref[span, :width].astype(jnp.float32)
        prod = short_ref[span, width : 2 * width].astype(jnp.float32) * short_ref[
            span, 2 * width :
        ].astype(jnp.float32)
        total = bias_ref[...] + taps_ref[KW - 1 : KW] * prod
        for back in range(1, KW):
            moved = pltpu.roll(prod, back, 0)
            for i in range(back):
                moved = jnp.where(row == i, before[KW - 1 - back + i], moved)
            total = total + taps_ref[KW - 1 - back : KW - back] * moved
        out_ref[span, :] = (gate * total).astype(jnp.bfloat16)
        return tuple(prod[rows - KW + 1 + i : rows - KW + 2 + i] for i in range(KW - 1))

    zero = jnp.zeros((1, width), jnp.float32)
    lax.fori_loop(0, length // rows, advance, (zero,) * (KW - 1))


def on_device(kernel, name, where, blocks, weights, shape, *operands):
    vmem = pl.BlockSpec(memory_space=pltpu.VMEM)
    count = len(blocks) + len(weights) + len(operands)
    return pl.pallas_call(
        functools.partial(
            kernel, rows=blocks[0].shape[0], counts=(len(blocks), len(weights))
        ),
        in_specs=[pl.BlockSpec(memory_space=pltpu.SMEM)] + [vmem] * count,
        out_specs=vmem,
        out_shape=jax.ShapeDtypeStruct(shape, jnp.bfloat16),
        scratch_shapes=[pltpu.VMEM((shape[0], weights[0].shape[2]), jnp.bfloat16)],
        name=name,
    )(where, *blocks, *weights, *operands)


def by_heads_shards(
    tokens,
    query_weight,
    forget_weight,
    value_weight,
    convolution_gate_weight,
    convolution_multiplier_weight,
    convolution_input_weight,
    gate_headroom,
    added_log_rate,
    initial_state,
    head_norm_gain,
    convolution_taps,
    convolution_bias,
    recurrence_output_weight,
    convolution_output_weight,
):
    n_sp = lax.axis_size("sp")
    n_fs = lax.axis_size("fs")
    place = lax.axis_index("sp")
    square = lax.axis_index("fs")
    where = jnp.stack([place, lax.axis_index("tp")])
    own_rows = tokens[0]
    rows, model = own_rows.shape
    row_count = query_weight.shape[0]
    out_cols = recurrence_output_weight.shape[1]

    def own(value, axis):
        size = value.shape[axis] // n_sp
        return lax.dynamic_slice_in_dim(value, place * size, size, axis)

    def columns(weights):
        parts = [w.reshape(row_count, n_sp, w.shape[1] // n_sp) for w in weights]
        return jnp.swapaxes(jnp.concatenate(parts, axis=2), 0, 1)

    first = columns((query_weight, forget_weight, value_weight))
    second = columns(
        (convolution_gate_weight, convolution_multiplier_weight, convolution_input_weight)
    )
    third = jnp.concatenate(
        [
            w.reshape(n_sp, -1, row_count, out_cols)
            for w in (recurrence_output_weight, convolution_output_weight)
        ],
        axis=1,
    )
    third = jnp.swapaxes(third, 1, 2).reshape(n_sp, row_count, -1)
    late = jnp.concatenate([second, third], axis=1)
    blocks = own_rows.reshape(rows, n_sp, n_fs, row_count)
    sorted_rows = jnp.concatenate(
        [lax.dynamic_index_in_dim(blocks, square ^ j, 2, False)[:, :, None] for j in range(n_fs)],
        axis=2,
    )
    sorted_rows = jnp.swapaxes(sorted_rows, 1, 2).reshape(rows, model)
    heads, positions = added_log_rate.shape[1:]
    rate_pieces = added_log_rate[0].reshape(n_sp, heads // n_sp, positions)
    rates = jnp.stack(exchange(for_offsets(rate_pieces, "sp"), "sp"))
    rates = jnp.swapaxes(rates, 1, 2).reshape(-1, heads // n_sp)

    first_got = exchange(for_offsets(first, "sp"), "sp")
    first_got[1], late = lax.optimization_barrier((first_got[1], late))
    late_got = exchange(for_offsets(late, "sp"), "sp")
    first_parts = square_gather(in_order(first_got, "sp"), "fs")
    late_got[1], sorted_rows = lax.optimization_barrier((late_got[1], sorted_rows))
    row_blocks = exchange([sorted_rows] * n_sp, "sp")
    late_mine = in_order(late_got, "sp")
    first_parts[1:], late_mine = lax.optimization_barrier((first_parts[1:], late_mine))
    late_parts = [late_mine] + [flip(late_mine, "fs", k) for k in range(1, n_fs)]

    first_parts[1:], row_blocks[1:] = lax.optimization_barrier((first_parts[1:], row_blocks[1:]))
    blocks = row_blocks + [flip(b, "tp", 1) for b in row_blocks]
    length = rows * len(blocks)

    head_cols = query_weight.shape[1] // n_sp
    conv_cols = convolution_gate_weight.shape[1] // n_sp
    rec_out = on_device(
        recurrence_kernel,
        "recurrence",
        where,
        blocks,
        first_parts,
        (length, head_cols),
        own(gate_headroom, 0)[None, :],
        rates,
        jnp.swapaxes(own(initial_state[0], 0), 1, 2),
        own(head_norm_gain, 0)[None, :],
    )
    rec_out, second_parts = lax.optimization_barrier((rec_out, late_parts))
    third_parts = [
        jnp.concatenate(jnp.split(p[:, row_count:], p.shape[2] // out_cols, axis=2), axis=1)
        for p in late_parts
    ]
    conv_out = on_device(
        convolution_kernel,
        "convolution",
        where,
        blocks,
        second_parts,
        (length, conv_cols),
        own(convolution_taps, 1),
        own(convolution_bias, 0)[None, :],
    )
    stacked = jnp.stack(third_parts)
    by_square = [lax.dynamic_index_in_dim(stacked, square ^ f, 0, False) for f in range(n_fs)]
    out_weight = jnp.concatenate(
        [by_square[f][s] for s in range(n_sp) for f in range(n_fs)], axis=1
    )
    other_weight = flip(out_weight, "tp", 1)
    mixed_in = jnp.concatenate([rec_out, conv_out], axis=1)
    from_other = flip(mixed_in[length // 2 :], "tp", 1)

    def outward(k):
        span = slice(k * rows, (k + 1) * rows)
        return (
            jnp.dot(mixed_in[span], out_weight, preferred_element_type=jnp.float32)
            + jnp.dot(from_other[span], other_weight, preferred_element_type=jnp.float32)
        ).astype(jnp.bfloat16)

    total = sum(
        part.astype(jnp.float32)
        for part in exchange([outward(k) for k in range(n_sp)], "sp")
    )
    return total.astype(jnp.bfloat16)[None]


def solution(mesh):
    in_specs = (
        P("fs", ("sp", "tp"), None),
        P(("sp", "fs"), "tp"),
        P(("sp", "fs"), "tp"),
        P(("sp", "fs"), "tp"),
        P(("sp", "fs"), "tp"),
        P(("sp", "fs"), "tp"),
        P(("sp", "fs"), "tp"),
        P("tp"),
        P("fs", "tp", "sp"),
        P("fs", "tp", None, None),
        P("tp"),
        P(None, "tp"),
        P("tp"),
        P("tp", ("sp", "fs")),
        P("tp", ("sp", "fs")),
    )
    out_specs = P("fs", ("sp", "tp"), None)
    sizes = dict(mesh.shape)

    def run(*arrays):
        heads = arrays[8].shape[1] // sizes["tp"]
        channels = arrays[4].shape[1] // sizes["tp"]
        by_heads = (
            (sizes["sp"], sizes["fs"], sizes["tp"]) == (4, 4, 2)
            and heads % sizes["sp"] == 0
            and channels % (128 * sizes["sp"]) == 0
        )
        return jax.shard_map(
            by_heads_shards if by_heads else shards,
            mesh=mesh,
            in_specs=in_specs,
            out_specs=out_specs,
            check_vma=False,
        )(*arrays)

    return run
```
